32 devices in a mesh: sp: 16 (over z, y, core), tp: 2 (over x).
Axes of the slice: x: 2, y: 2, z: 4, core: 2. Of those that a mesh axis runs over, the one named last changes fastest.
Arguments:
- latent: bfloat16 [8192, 2048], P(('sp', 'tp')), may hold values from -6 to 6
- context: bfloat16 [1024, 2048], P('sp'), may hold values from -6 to 6
- condition: float32 [2048], replicated, may hold values from -6 to 6
- context_condition: float32 [2048], replicated, may hold values from -6 to 6
- modulation_weight: bfloat16 [2048, 3, 2048], P('sp', None, 'tp'), may hold values from -0.125 to 0.125
- norm_gain: float32 [2048], replicated, may hold values from 0.1 to 1.9
- query_weight: bfloat16 [2048, 2048], P(None, 'tp'), may hold values from -0.125 to 0.125
- key_weight: bfloat16 [2048, 2048], P(None, 'tp'), may hold values from -0.125 to 0.125
- value_weight: bfloat16 [2048, 2048], P(None, 'tp'), may hold values from -0.125 to 0.125
- log_decay: float32 [2, 32], P(None, 'tp')
- head_gain: float32 [2048], P('tp'), may hold values from 0.1 to 1.9
- output_weight: bfloat16 [2048, 2048], P('sp'), may hold values from -0.125 to 0.125
Outputs:
- output: bfloat16 [8192, 2048], P(('sp', 'tp'))
The draws below stay inside these ranges and needn't reach their ends.
All inputs are finite; a program needn't handle non-finite values.
Results may differ from the reference program's by a relative error of at most 0.0065.
Values may be sent and summed in bfloat16 or wider, within the bound.
A program may use at most 128 MiB of HBM per device.

```python
import jax
import jax.numpy as jnp
from jax import lax

D = 2048
HEADS = 32
HEAD = 64
BLOCK = 128
CTX = 1024
TOK_DEV = 512
TOKENS = 8192


def draw_log_decay(key, part):
    decays = []
    for direction in range(2):
        branch_key = jax.random.fold_in(key, 37 + direction)
        order_key, fast_key, slow_key, middle_key = jax.random.split(branch_key, 4)
        ranking = jax.random.permutation(order_key, HEADS)
        fast_count = max(1, HEADS // 4)
        middle_count = max(1, HEADS // 4)
        fast_spread = jax.random.uniform(fast_key, (HEADS,), jnp.float32)
        slow_spread = jax.random.uniform(slow_key, (HEADS,), jnp.float32)
        middle_spread = jax.random.uniform(middle_key, (HEADS,), jnp.float32, jnp.log(0.1), jnp.log(4.0))
        fast_rate = -1.0 / (BLOCK * (0.25 + 0.5 * fast_spread))
        middle_rate = -jnp.exp(middle_spread) / TOK_DEV
        slow_rate = jnp.log(0.1) * (0.2 + 0.8 * slow_spread) / TOKENS
        chosen = jnp.where(ranking < fast_count, fast_rate, jnp.where(ranking < fast_count + middle_count, middle_rate, slow_rate))
        decays.append(chosen)
    return jnp.stack(decays).astype(jnp.float32)


def level_of(key, dims, cuts, low, largest):
    factor_of, own = 1.0, jax.random.fold_in(key, 6)
    for position, blocks in cuts:
        draws = jnp.exp(jax.random.uniform(jax.random.fold_in(own, position), (blocks,), jnp.float32, low / len(cuts), largest / len(cuts)))
        factor_of = factor_of * jnp.repeat(draws, dims[position] // blocks).reshape([-1 if axis == position else 1 for axis in range(len(dims))])
    return factor_of


def scatter_about(rng, shape, scale, limit, cuts=(), kind=jnp.bfloat16):
    values = scale * jax.random.normal(rng, shape, jnp.float32)
    if cuts:
        values = values * level_of(rng, shape, cuts, -0.22, 0.18)
    return jnp.clip(values, -limit, limit).astype(kind)


def setup_inputs(seed: int = 0) -> dict:
    key_of = jax.random.split(jax.random.key(seed), 13)
    return {
        "latent": scatter_about(key_of[0], (TOKENS, D), 1.0, 6.0, ((0, 32),)),
        "context": scatter_about(key_of[1], (CTX, D), 1.0, 6.0, ((0, 16),)),
        "condition": scatter_about(key_of[2], (D,), 1.0, 6.0, (), jnp.float32),
        "context_condition": scatter_about(key_of[3], (D,), 1.0, 6.0, (), jnp.float32),
        "modulation_weight": scatter_about(key_of[4], (D, 3, D), D ** -0.5, 0.125, ((0, 16), (2, 2))),
        "norm_gain": jnp.clip(1.0 + 0.18 * jax.random.normal(key_of[5], (D,), jnp.float32), 0.1, 1.9),
        "query_weight": scatter_about(key_of[6], (D, HEADS * HEAD), D ** -0.5, 0.125, ((1, 2),)),
        "key_weight": scatter_about(key_of[7], (D, HEADS * HEAD), D ** -0.5, 0.125, ((1, 2),)),
        "value_weight": scatter_about(key_of[8], (D, HEADS * HEAD), D ** -0.5, 0.125, ((1, 2),)),
        "log_decay": draw_log_decay(jax.random.fold_in(key_of[12], 71), 0),
        "head_gain": jnp.clip(1.0 + 0.18 * jax.random.normal(key_of[10], (HEADS * HEAD,), jnp.float32), 0.1, 1.9),
        "output_weight": scatter_about(key_of[11], (HEADS * HEAD, D), (HEADS * HEAD) ** -0.5, 0.125, ((0, 16),)),
    }


EPSILON = 1e-06
ROTARY_BASE = 10000.0
MAXIMAL_ACCURACY = lax.Precision.HIGHEST

def rotation_tables(positions):
    half_size = HEAD // 2
    frequency = 1.0 / ROTARY_BASE ** jnp.linspace(0.0, 1.0, half_size, dtype=jnp.float32)
    angles = positions[:, None] * frequency[None, :]
    return (jnp.cos(angles), jnp.sin(angles))

def rotate(projected, positions):
    cos_table, sin_table = rotation_tables(positions)
    half_size = HEAD // 2
    lower_half = projected[..., :half_size]
    upper_half = projected[..., half_size:]
    cos_table = cos_table[:, None, :]
    sin_table = sin_table[:, None, :]
    return jnp.concatenate([lower_half * cos_table - upper_half * sin_table, lower_half * sin_table + upper_half * cos_table], axis=-1)

def modulated(rows, gain, shift, scale):
    widened = rows.astype(jnp.float32)
    scaled = widened * lax.rsqrt(lax.optimization_barrier(jnp.mean(widened * widened, axis=-1, keepdims=True)) + EPSILON)
    return (scaled * gain * (1.0 + scale) + shift).astype(jnp.bfloat16)

def project(rows, weight):
    return jnp.dot(rows, weight, preferred_element_type=jnp.float32).reshape(rows.shape[0], HEADS, HEAD)

def sweep(queries, keys, values, log_rate, start_state):
    length = queries.shape[0]
    blocks = length // BLOCK
    offsets = jnp.arange(BLOCK, dtype=jnp.float32)
    distance = offsets[:, None] - offsets[None, :]
    decay_mask = jnp.where(distance >= 0, jnp.exp(log_rate[:, None, None] * jnp.maximum(distance, 0.0)[None]), 0.0)
    query_decay = jnp.exp(log_rate[:, None] * (offsets + 1.0)[None]).T
    key_decay = jnp.exp(log_rate[:, None] * (BLOCK - 1.0 - offsets)[None]).T
    block_decay = jnp.exp(log_rate * BLOCK)
    query_blocks = queries.reshape(blocks, BLOCK, HEADS, HEAD)
    key_blocks = keys.reshape(blocks, BLOCK, HEADS, HEAD)
    value_blocks = values.reshape(blocks, BLOCK, HEADS, HEAD)

    def block_step(state, pieces):
        broad_query_matrix = pieces[0].astype(jnp.float32)
        broad_key_matrix = pieces[1].astype(jnp.float32)
        broad_value_matrix = pieces[2].astype(jnp.float32)
        affinity_scores = jnp.einsum('nsg,psg->snp', broad_query_matrix, broad_key_matrix, precision=MAXIMAL_ACCURACY)
        weight_tensors = lax.optimization_barrier((affinity_scores * decay_mask).astype(jnp.bfloat16)).astype(jnp.float32)
        inside_block = jnp.einsum('ngj,jnr->gnr', weight_tensors, broad_value_matrix, precision=MAXIMAL_ACCURACY)
        carried = jnp.einsum('lhd,hde->lhe', broad_query_matrix, state, precision=MAXIMAL_ACCURACY) * query_decay[:, :, None]
        update = jnp.einsum('lhd,lhe->hde', broad_key_matrix * key_decay[:, :, None], broad_value_matrix, precision=MAXIMAL_ACCURACY)
        return (block_decay[:, None, None] * state + update, inside_block + carried)
    final_state, outputs = lax.scan(block_step, start_state, (query_blocks, key_blocks, value_blocks))
    return outputs.reshape(length, HEADS, HEAD)

def reference(latent, context, condition, context_condition, modulation_weight, norm_gain, query_weight, key_weight, value_weight, log_decay, head_gain, output_weight):
    activated = jax.nn.silu(jnp.stack([condition, context_condition])).astype(jnp.bfloat16)
    modulation = jnp.dot(activated, modulation_weight.reshape(D, 3 * D), preferred_element_type=jnp.float32).reshape(2, 3, D)
    normed = modulated(latent, norm_gain, modulation[0, 0], modulation[0, 1])
    context_normed = modulated(context, norm_gain, modulation[1, 0], modulation[1, 1])
    latent_positions = CTX + jnp.arange(TOKENS, dtype=jnp.float32)
    context_positions = jnp.arange(CTX, dtype=jnp.float32)
    queries = (rotate(project(normed, query_weight), latent_positions) * HEAD ** (-0.5)).astype(jnp.bfloat16)
    keys = rotate(project(normed, key_weight), latent_positions).astype(jnp.bfloat16)
    values = project(normed, value_weight).astype(jnp.bfloat16)
    context_keys = rotate(project(context_normed, key_weight), context_positions).astype(jnp.bfloat16)
    context_values = project(context_normed, value_weight).astype(jnp.bfloat16)
    broad_key_matrix = context_keys.astype(jnp.float32)
    broad_value_matrix = context_values.astype(jnp.float32)
    forward_weight = jnp.exp(log_decay[0][None, :] * (CTX - 1.0 - context_positions)[:, None])
    backward_weight = jnp.exp(log_decay[1][None, :] * context_positions[:, None])
    start_forward = jnp.einsum('jhd,jhe->hde', broad_key_matrix * forward_weight[:, :, None], broad_value_matrix, precision=MAXIMAL_ACCURACY)
    start_backward = jnp.einsum('jhd,jhe->hde', broad_key_matrix * backward_weight[:, :, None], broad_value_matrix, precision=MAXIMAL_ACCURACY)
    forward = sweep(queries, keys, values, log_decay[0], start_forward)
    backward = jnp.flip(sweep(jnp.flip(queries, 0), jnp.flip(keys, 0), jnp.flip(values, 0), log_decay[1], start_backward), 0)
    combined = forward + backward
    centre = lax.optimization_barrier(jnp.mean(combined, axis=-1, keepdims=True))
    spread = lax.optimization_barrier(jnp.mean(jnp.square(combined - centre), axis=-1, keepdims=True))
    retained = ((combined - centre) * lax.rsqrt(spread + EPSILON) * head_gain.reshape(HEADS, HEAD)).astype(jnp.bfloat16)
    retained = retained.reshape(TOKENS, HEADS * HEAD)
    mixed = jnp.dot(retained, output_weight, preferred_element_type=jnp.float32)
    return (latent.astype(jnp.float32) + modulation[0, 2] * mixed).astype(jnp.bfloat16)
```

```python
import functools

import jax
import jax.numpy as jnp
from jax import lax
from jax.experimental import pallas as pl
from jax.experimental.pallas import tpu as pltpu
from jax.sharding import PartitionSpec as P

HEAD = 64
CTX = 1024
LANES = 128
EPSILON = 1e-06
ROTARY_BASE = 10000.0
MESH = pl.DeviceIdType.MESH
F32 = jnp.float32
BF16 = jnp.bfloat16


def rotation_tables(positions):
    half_size = HEAD // 2
    frequency = 1.0 / ROTARY_BASE ** jnp.linspace(0.0, 1.0, half_size, dtype=F32)
    angles = positions[:, None] * frequency[None, :]
    cos, sin = jnp.cos(angles), jnp.sin(angles)
    return (
        jnp.concatenate([cos] * 4, axis=1),
        jnp.concatenate([-sin, sin, -sin, sin], axis=1),
    )


def dot(a, b, dims=((1,), (0,))):
    return lax.dot_general(a, b, (dims, ((), ())), preferred_element_type=F32)


def loop(count, body):
    def step(i, carry):
        body(i)
        return carry

    lax.fori_loop(0, count, step, 0)


def swap_halves(u, lane):
    return jnp.where(lane % HEAD < HEAD // 2, pltpu.roll(u, LANES - 32, 1), pltpu.roll(u, 32, 1))


def kernel(
    nsp,
    ntp,
    owned,
    latent,
    context,
    part,
    gain,
    wq,
    wk,
    wv,
    decay,
    row_decay,
    head_gain,
    wo_own,
    cos,
    sin,
    ccos,
    csin,
    out,
    lat,
    xn,
    cn,
    wq_v,
    wk_v,
    wv_v,
    wo,
    mrecv,
    mred,
    mod,
    modrow,
    q,
    k,
    v,
    ck,
    cv,
    st_send,
    st_recv,
    scan,
    en_send,
    en_recv,
    local,
    ret,
    got,
    acc,
    load_sem,
    lat_send_sem,
    lat_recv_sem,
    ms_sem,
    mr_sem,
    bs_sem,
    br_sem,
    ss_sem,
    sr_sem,
    es_sem,
    er_sem,
    gs_sem,
    gr_sem,
    wo_send_sem,
    wo_recv_sem,
):
    s = lax.axis_index("sp")
    t = lax.axis_index("tp")
    rows, dim = latent.shape
    tok = rows * ntp
    width = wq.shape[1]
    pairs = width // LANES
    crow = context.shape[0]
    nch = part.shape[0]
    owners = width // owned
    block = wo_own.shape[0]
    nz = nsp // 4
    z, y, c = s // 4, (s // 2) % 2, s % 2

    def remote(src, dst, send, recv, where):
        return pltpu.make_async_remote_copy(
            src_ref=src,
            dst_ref=dst,
            send_sem=send,
            recv_sem=recv,
            device_id=where,
            device_id_type=MESH,
        )

    loads = [
        pltpu.make_async_copy(latent, lat.at[t], load_sem.at[0]),
        pltpu.make_async_copy(wk, wk_v, load_sem.at[1]),
        pltpu.make_async_copy(wv, wv_v, load_sem.at[2]),
        pltpu.make_async_copy(wq, wq_v, load_sem.at[3]),
        pltpu.make_async_copy(wo_own, wo.at[s], load_sem.at[4]),
    ]

    def part_copy(j):
        return remote(part.at[j], mrecv.at[s], ms_sem.at[j], mr_sem.at[s], (j, t))

    for j in range(nch):
        @pl.when(s != j)
        def _():
            part_copy(j).start()

        @pl.when(s == j)
        def _():
            mrecv[j] = part[j]

    def lat_copy(d):
        peer = (t + d) % ntp
        return remote(latent, lat.at[t], lat_send_sem.at[d], lat_recv_sem.at[t], (s, peer))

    for d in range(1, ntp):
        lat_copy(d).start()
    for copy in loads:
        copy.start()

    def wo_copy(b, kind, src=None):
        if kind == 0:
            where = s + 4
        elif kind == 1:
            where = s - 4
        elif kind == 2:
            where = z * 4 + (1 - y) * 2 + c
        else:
            where = z * 4 + y * 2 + (1 - c)
        ref = wo.at[b] if src is None else src
        return remote(ref, wo.at[b], wo_send_sem.at[b, kind], wo_recv_sem.at[b], (where, t))

    def wo_arrived(b):
        remote(wo.at[b], wo.at[b], wo_send_sem.at[b, 0], wo_recv_sem.at[b], (s, t)).wait_recv()

    def up_ok(cond=True):
        return (z < nz - 1) & cond

    def wo_own_sends(act):
        @pl.when(z < nz - 1)
        def _():
            act(wo_copy(s, 0, wo_own))

        @pl.when(z > 0)
        def _():
            act(wo_copy(s, 1, wo_own))

        act(wo_copy(s, 2, wo_own))
        act(wo_copy(s, 3, wo_own))

    wo_own_sends(lambda copy: copy.start())

    def wo_y_arrived(distance):
        def one(zz):
            b = zz * 4 + (1 - y) * 2 + c
            wo_arrived(b)
            wo_copy(b, 3).start()

        if distance == 0:
            one(z)
            return

        @pl.when(z - distance >= 0)
        def _():
            one(z - distance)

        @pl.when(z + distance < nz)
        def _():
            one(z + distance)

    def wo_z_forward(distance, act, wait):
        @pl.when(z - distance >= 0)
        def _():
            b = s - 4 * distance
            if wait:
                wo_arrived(b)

            @pl.when(z < nz - 1)
            def _():
                act(wo_copy(b, 0))

            act(wo_copy(b, 2))
            act(wo_copy(b, 3))

        @pl.when(z + distance < nz)
        def _():
            b = s + 4 * distance
            if wait:
                wo_arrived(b)

            @pl.when(z > 0)
            def _():
                act(wo_copy(b, 1))

            act(wo_copy(b, 2))
            act(wo_copy(b, 3))

    def wo_step(distance):
        wo_z_forward(distance, lambda copy: copy.start(), True)

    def to_all(act):
        def one(i):
            where = (s + i // ntp) % nsp, (t + i % ntp) % ntp

            @pl.when(i > 0)
            def _():
                act(remote(mred, mod.at[t * nch + s], bs_sem.at[i], br_sem.at[t * nch + s], where))

        loop(nsp * ntp, one)

    @pl.when(s < nch)
    def _():
        def arrived(j):
            @pl.when(j != s)
            def _():
                remote(part.at[0], mrecv.at[j], ms_sem.at[0], mr_sem.at[j], (j, t)).wait_recv()

        loop(nsp, arrived)
        total = mrecv[0]
        for j in range(1, nsp):
            total = total + mrecv[j]
        mred[...] = total
        mod[t * nch + s] = total
        to_all(lambda copy: copy.start())

    for j in range(nch * ntp):
        @pl.when(t * nch + s != j)
        def _():
            remote(mred, mod.at[j], bs_sem.at[0], br_sem.at[j], (s, t)).wait_recv()

        @pl.when((t * nch + s == j) & (s >= nch))
        def _():
            remote(mred, mod.at[j], bs_sem.at[0], br_sem.at[j], (s, t)).wait_recv()

        modrow[:, j * LANES : (j + 1) * LANES] = mod[j]

    def normalise(src, dst, count, row):
        step = min(count, 64)

        def one(i):
            at = pl.ds(pl.multiple_of(i * step, step), step)
            x = src(at).astype(F32)
            inverse = lax.rsqrt(jnp.mean(x * x, axis=-1, keepdims=True) + EPSILON)
            dst[at, :] = (
                x * inverse * gain[...] * (1.0 + modrow[row + 1 : row + 2, :])
                + modrow[row : row + 1, :]
            ).astype(BF16)

        loop(count // step, one)

    lane_r = lax.broadcasted_iota(jnp.int32, (rows, LANES), 1)
    lane_c = lax.broadcasted_iota(jnp.int32, (crow, LANES), 1)
    tile = min(width, 256)

    normalise(lambda at: context[at, :], cn, crow, 3)
    loads[0].wait()
    loads[1].wait()
    loads[2].wait()

    def context_tile(j):
        at = pl.ds(pl.multiple_of(j * tile, tile), tile)
        kk = dot(cn[...], wk_v[:, at])
        cv[:, at] = dot(cn[...], wv_v[:, at]).astype(BF16)
        for h in range(tile // LANES):
            u = kk[:, h * LANES : (h + 1) * LANES]
            r = u * ccos[...] + swap_halves(u, lane_c) * csin[...]
            ck[:, pl.ds(pl.multiple_of(j * tile + h * LANES, LANES), LANES)] = r.astype(BF16)

    loop(width // tile, context_tile)
    loads[3].wait()

    def project(d):
        src = (t + d) % ntp
        here = pl.ds(pl.multiple_of(src * rows, rows), rows)

        @pl.when(d > 0)
        def _():
            remote(latent, lat.at[src], lat_send_sem.at[0], lat_recv_sem.at[src], (s, t)).wait_recv()

        normalise(lambda at: lat[src, at, :], xn, rows, 0)

        def tile_step(j):
            at = pl.ds(pl.multiple_of(j * tile, tile), tile)
            v[here, at] = dot(xn[...], wv_v[:, at]).astype(BF16)
            cc, sn = cos[here, :], sin[here, :]
            for w_v, dst, scale in ((wk_v, k, None), (wq_v, q, HEAD ** (-0.5))):
                full = dot(xn[...], w_v[:, at])
                for h in range(tile // LANES):
                    u = full[:, h * LANES : (h + 1) * LANES]
                    r = u * cc + swap_halves(u, lane_r) * sn
                    if scale is not None:
                        r = r * scale
                    dst[here, pl.ds(pl.multiple_of(j * tile + h * LANES, LANES), LANES)] = r.astype(
                        BF16
                    )

        loop(width // tile, tile_step)

    project(0)
    wo_y_arrived(0)
    for distance in range(1, nz // 2):
        wo_step(distance)
    if ntp > 1:
        loop(ntp - 1, lambda d: project(d + 1))
    for distance in range(max(nz // 2, 1), nz):
        wo_step(distance)
    for distance in range(1, nz // 2):
        wo_y_arrived(distance)

    row_s = lax.broadcasted_iota(jnp.int32, (LANES, LANES), 0)
    lane_s = lax.broadcasted_iota(jnp.int32, (LANES, LANES), 1)
    lane_1 = lax.broadcasted_iota(jnp.int32, (1, LANES), 1)
    time_t = lax.broadcasted_iota(jnp.int32, (tok, LANES), 0).astype(F32)
    time_c = lax.broadcasted_iota(jnp.int32, (crow, LANES), 0).astype(F32)

    def rate(direction, p):
        return jnp.where(lane_1 < HEAD, decay[direction, 2 * p], decay[direction, 2 * p + 1])

    def pack(forward, backward):
        return jnp.where(
            lane_s < HEAD,
            jnp.where(row_s < HEAD, forward, pltpu.roll(forward, HEAD, 1)),
            jnp.where(row_s < HEAD, pltpu.roll(backward, HEAD, 1), backward),
        ).astype(BF16)

    def states(p):
        at = pl.ds(pl.multiple_of(p * LANES, LANES), LANES)
        ahead, behind = rate(0, p), rate(1, p)
        for which, keys, values, time in ((0, k, v, time_t), (1, ck, cv, time_c)):
            length = time.shape[0]
            kk = keys[:, at].astype(F32)
            vv = values[:, at]
            weighted = (kk * jnp.exp(ahead * (length - 1.0 - time))).astype(BF16)
            forward = dot(weighted, vv, ((0,), (0,)))
            weighted = (kk * jnp.exp(behind * time)).astype(BF16)
            backward = dot(weighted, vv, ((0,), (0,)))
            packed = pack(forward, backward)
            for i in range(LANES // owned):
                st_send[p * (LANES // owned) + i, which] = packed[i * owned : (i + 1) * owned, :]

    loop(pairs, states)

    def state_copy(j):
        return remote(st_send.at[j], st_recv.at[s], ss_sem.at[j], sr_sem.at[s], (j, t))

    def send_states(d):
        j = (s + d) % nsp

        @pl.when((j < owners) & (d > 0))
        def _():
            state_copy(j).start()

    loop(nsp, send_states)

    @pl.when(s < owners)
    def _():
        st_recv[s] = st_send[s]

    row_q = lax.broadcasted_iota(jnp.int32, (tok, tok), 0)
    col_q = lax.broadcasted_iota(jnp.int32, (tok, tok), 1)
    lane_t = lax.broadcasted_iota(jnp.int32, (tok, LANES), 1)

    def inside(p):
        at = pl.ds(pl.multiple_of(p * LANES, LANES), LANES)
        qq, kk, vv = q[:, at], k[:, at], v[:, at]
        gap = (row_q - col_q).astype(F32)
        halves = []
        for a in range(2):
            ahead, behind = decay[0, 2 * p + a], decay[1, 2 * p + a]
            mine = (lane_t < HEAD) if a == 0 else (lane_t >= HEAD)
            scores = dot(jnp.where(mine, qq.astype(F32), 0.0).astype(BF16), kk, ((1,), (1,)))
            mask = jnp.where(gap == 0.0, 2.0, jnp.exp(jnp.where(gap > 0.0, ahead, -behind) * gap))
            halves.append(dot((scores * mask).astype(BF16), vv))
        local[:, at] = jnp.where(lane_t < HEAD, halves[0], halves[1])

    first = (pairs + 1) // 2
    loop(first, inside)

    lane_o = lax.broadcasted_iota(jnp.int32, (owned, LANES), 1)

    def enter_copy(j):
        return remote(en_send.at[j], en_recv.at[s], es_sem.at[j], er_sem.at[s], (j, t))

    @pl.when(s < owners)
    def _():
        def arrived(j):
            @pl.when(j != s)
            def _():
                remote(
                    st_send.at[0], st_recv.at[j], ss_sem.at[0], sr_sem.at[j], (j, t)
                ).wait_recv()

        loop(nsp, arrived)
        latent_step = jnp.exp(row_decay[...] * float(tok))
        context_step = jnp.exp(row_decay[...] * float(crow))

        def gather_forward(j, carry):
            return context_step * carry + st_recv[j, 1].astype(F32)

        def gather_backward(i, carry):
            return context_step * carry + st_recv[nsp - 1 - i, 1].astype(F32)

        zero = jnp.zeros((owned, LANES), F32)
        start = jnp.where(
            lane_o < HEAD,
            lax.fori_loop(0, nsp, gather_forward, zero),
            lax.fori_loop(0, nsp, gather_backward, zero),
        )

        def forward_step(i, carry):
            scan[i] = carry
            return latent_step * carry + st_recv[i, 0].astype(F32)

        lax.fori_loop(0, nsp, forward_step, start)

        def backward_step(n, carry):
            i = nsp - 1 - n
            en_send[i] = jnp.where(lane_o < HEAD, scan[i], carry).astype(BF16)
            return latent_step * carry + st_recv[i, 0].astype(F32)

        lax.fori_loop(0, nsp, backward_step, start)

        def send(j):
            @pl.when(j != s)
            def _():
                enter_copy(j).start()

        loop(nsp, send)
        en_recv[s] = en_send[s]

    loop(pairs - first, lambda p: inside(p + first))
    for distance in range(max(nz // 2, 1), nz):
        wo_y_arrived(distance)

    def entered(j):
        @pl.when(j != s)
        def _():
            remote(en_send.at[0], en_recv.at[j], es_sem.at[0], er_sem.at[j], (j, t)).wait_recv()

    loop(owners, entered)

    averaging = jnp.where((row_s < HEAD) == (lane_s < HEAD), 1.0 / HEAD, 0.0).astype(BF16)

    def head_mean(x):
        high = x.astype(BF16)
        low = (x - high.astype(F32)).astype(BF16)
        return dot(high, averaging) + dot(low, averaging)

    def ret_copy(d, p):
        peer = (t + d) % ntp
        at = pl.ds(pl.multiple_of(p * LANES, LANES), LANES)
        return remote(
            ret.at[pl.ds(pl.multiple_of(peer * rows, rows), rows), at],
            got.at[t, :, at],
            gs_sem.at[d, p],
            gr_sem.at[t, p],
            (s, peer),
        )

    def finish(p):
        at = pl.ds(pl.multiple_of(p * LANES, LANES), LANES)
        per = LANES // owned
        packed = jnp.concatenate([en_recv[p * per + i].astype(F32) for i in range(per)], axis=0)
        turned = pltpu.roll(packed, HEAD, 1)
        top = (row_s < HEAD) & (lane_s < HEAD)
        bottom = (row_s >= HEAD) & (lane_s >= HEAD)
        forward = jnp.where(top, packed, jnp.where(bottom, turned, 0.0)).astype(BF16)
        backward = jnp.where(top, turned, jnp.where(bottom, packed, 0.0)).astype(BF16)
        qq = q[:, at]
        o = (
            local[:, at]
            + dot(qq, forward) * jnp.exp(rate(0, p) * (time_t + 1.0))
            + dot(qq, backward) * jnp.exp(rate(1, p) * (float(tok) - time_t))
        )
        o = o - head_mean(o)
        spread = head_mean(o * o)
        ret[:, at] = (o * lax.rsqrt(spread + EPSILON) * head_gain[:, at]).astype(BF16)
        for d in range(1, ntp):
            ret_copy(d, p).start()
        got[t, :, at] = ret[pl.ds(pl.multiple_of(t * rows, rows), rows), at]

    loop(pairs, finish)

    for zz in range(nz):
        for yy in range(2):
            wo_arrived(zz * 4 + yy * 2 + (1 - c))
    loads[4].wait()

    per_head_block = width // block
    cols = min(dim, 512)

    def product(src, at):
        weight = wo[pl.ds(src * per_head_block, per_head_block), :, at]
        return dot(got[src], weight.reshape(width, cols))

    def own_product(n):
        at = pl.ds(pl.multiple_of(n * cols, cols), cols)
        acc[:, at] = product(t, at)

    loop(dim // cols, own_product)
    for d in range(1, ntp):
        src = (t + d) % ntp

        def got_wait(p):
            at = pl.ds(pl.multiple_of(p * LANES, LANES), LANES)
            remote(
                ret.at[pl.ds(0, rows), at],
                got.at[src, :, at],
                gs_sem.at[0, p],
                gr_sem.at[src, p],
                (s, t),
            ).wait_recv()

        loop(pairs, got_wait)
        last = d == ntp - 1

        def peer_product(n):
            at = pl.ds(pl.multiple_of(n * cols, cols), cols)
            total = acc[:, at] + product(src, at)
            if last:
                out[:, at] = (lat[t, :, at].astype(F32) + modrow[2:3, at] * total).astype(BF16)
            else:
                acc[:, at] = total

        loop(dim // cols, peer_product)

    for j in range(nch):
        @pl.when(s != j)
        def _():
            part_copy(j).wait_send()
    for d in range(1, ntp):
        lat_copy(d).wait_send()

    @pl.when(s < nch)
    def _():
        to_all(lambda copy: copy.wait_send())

    def states_left(d):
        j = (s + d) % nsp

        @pl.when((j < owners) & (d > 0))
        def _():
            state_copy(j).wait_send()

    loop(nsp, states_left)

    @pl.when(s < owners)
    def _():
        def left(j):
            @pl.when(j != s)
            def _():
                enter_copy(j).wait_send()

        loop(nsp, left)

    for d in range(1, ntp):
        loop(pairs, lambda p: ret_copy(d, p).wait_send())
    wo_own_sends(lambda copy: copy.wait_send())
    for distance in range(1, nz):
        wo_z_forward(distance, lambda copy: copy.wait_send(), False)
    for zz in range(nz):
        wo_copy(zz * 4 + (1 - y) * 2 + c, 3).wait_send()


def per_device(
    latent,
    context,
    condition,
    context_condition,
    modulation_weight,
    norm_gain,
    query_weight,
    key_weight,
    value_weight,
    log_decay,
    head_gain,
    output_weight,
):
    nsp, ntp = lax.axis_size("sp"), lax.axis_size("tp")
    s = lax.axis_index("sp")
    rows, dim = latent.shape
    tok = rows * ntp
    crow = context.shape[0]
    width = query_weight.shape[1]
    pairs = width // LANES
    owned = max(width // nsp, 16)
    owners = width // owned
    activated = jax.nn.silu(jnp.stack([condition, context_condition])).astype(BF16)
    entries, kinds, cols = modulation_weight.shape
    own_inputs = lax.dynamic_slice_in_dim(activated, s * entries, entries, 1)
    partial = jnp.einsum(
        "ce,erd->crd", own_inputs, modulation_weight, preferred_element_type=F32
    ).reshape(2 * kinds, cols)
    nch = cols // LANES
    part = jnp.pad(partial, ((0, 8 - 2 * kinds), (0, 0))).reshape(8, nch, LANES).transpose(1, 0, 2)
    cos, sin = rotation_tables(
        CTX + (s * tok).astype(F32) + jnp.arange(tok, dtype=F32)
    )
    ccos, csin = rotation_tables((s * crow).astype(F32) + jnp.arange(crow, dtype=F32))
    held = (s * owned + jnp.arange(owned)) // HEAD
    mine = jnp.take(log_decay, jnp.minimum(held, width // HEAD - 1), axis=1)
    row_decay = jnp.repeat(mine.T, HEAD, axis=1)
    vmem = pl.BlockSpec(memory_space=pltpu.VMEM)
    anywhere = pl.BlockSpec(memory_space=pl.ANY)
    smem = pl.BlockSpec(memory_space=pltpu.SMEM)
    dma = pltpu.SemaphoreType.DMA
    scratch = [
        pltpu.VMEM((ntp, rows, dim), BF16),
        pltpu.VMEM((rows, dim), BF16),
        pltpu.VMEM((crow, dim), BF16),
        pltpu.VMEM((dim, width), BF16),
        pltpu.VMEM((dim, width), BF16),
        pltpu.VMEM((dim, width), BF16),
        pltpu.VMEM((nsp,) + output_weight.shape, BF16),
        pltpu.VMEM((nsp, 8, LANES), F32),
        pltpu.VMEM((8, LANES), F32),
        pltpu.VMEM((ntp * nch, 8, LANES), F32),
        pltpu.VMEM((8, dim), F32),
        pltpu.VMEM((tok, width), BF16),
        pltpu.VMEM((tok, width), BF16),
        pltpu.VMEM((tok, width), BF16),
        pltpu.VMEM((crow, width), BF16),
        pltpu.VMEM((crow, width), BF16),
        pltpu.VMEM((owners, 2, owned, LANES), BF16),
        pltpu.VMEM((nsp, 2, owned, LANES), BF16),
        pltpu.VMEM((nsp, owned, LANES), F32),
        pltpu.VMEM((nsp, owned, LANES), BF16),
        pltpu.VMEM((owners, owned, LANES), BF16),
        pltpu.VMEM((tok, width), F32),
        pltpu.VMEM((tok, width), BF16),
        pltpu.VMEM((ntp, rows, width), BF16),
        pltpu.VMEM((rows, dim), F32),
        dma((5,)),
        dma((ntp,)),
        dma((ntp,)),
        dma((nch,)),
        dma((nsp,)),
        dma((nsp * ntp,)),
        dma((ntp * nch,)),
        dma((owners,)),
        dma((nsp,)),
        dma((nsp,)),
        dma((owners,)),
        dma((ntp, pairs)),
        dma((ntp, pairs)),
        dma((nsp, 4)),
        dma((nsp,)),
    ]
    return pl.pallas_call(
        functools.partial(kernel, nsp, ntp, owned),
        out_shape=jax.ShapeDtypeStruct((rows, dim), BF16),
        in_specs=[anywhere, vmem, vmem, vmem, anywhere, anywhere, anywhere, smem]
        + [vmem, vmem, anywhere]
        + [vmem] * 4,
        out_specs=vmem,
        scratch_shapes=scratch,
        compiler_params=pltpu.CompilerParams(
            has_side_effects=True, vmem_limit_bytes=66_000_000
        ),
    )(
        latent,
        context,
        part,
        norm_gain[None],
        query_weight,
        key_weight,
        value_weight,
        log_decay,
        row_decay,
        head_gain[None],
        output_weight,
        cos,
        sin,
        ccos,
        csin,
    )


def solution(mesh):
    in_specs = (
        P(("sp", "tp"), None),
        P("sp", None),
        P(),
        P(),
        P("sp", None, "tp"),
        P(),
        P(None, "tp"),
        P(None, "tp"),
        P(None, "tp"),
        P(None, "tp"),
        P("tp"),
        P("sp", None),
    )
    out_specs = P(("sp", "tp"), None)
    return jax.shard_map(
        per_device, mesh=mesh, in_specs=in_specs, out_specs=out_specs, check_vma=False
    )
```

```python
import functools

import jax
import jax.numpy as jnp
from jax import lax
from jax.experimental import pallas as pl
from jax.experimental.pallas import tpu as pltpu
from jax.sharding import PartitionSpec as P

HEAD = 64
CTX = 1024
LANES = 128
EPSILON = 1e-06
ROTARY_BASE = 10000.0
MESH = pl.DeviceIdType.MESH
F32 = jnp.float32
BF16 = jnp.bfloat16


def rotation_tables(positions):
    half_size = HEAD // 2
    frequency = 1.0 / ROTARY_BASE ** jnp.linspace(0.0, 1.0, half_size, dtype=F32)
    lane = jnp.arange(LANES)
    angles = positions[:, None] * jnp.tile(frequency, LANES // half_size)[None, :]
    sign = jnp.where(lane % HEAD < half_size, -1.0, 1.0).astype(F32)
    return jnp.cos(angles), jnp.sin(angles) * sign[None, :]


def dot(a, b, dims=((1,), (0,))):
    return lax.dot_general(a, b, (dims, ((), ())), preferred_element_type=F32)


def loop(count, body):
    def step(i, carry):
        body(i)
        return carry

    lax.fori_loop(0, count, step, 0)


def swap_halves(u, lane):
    return jnp.where(lane % HEAD < HEAD // 2, pltpu.roll(u, LANES - 32, 1), pltpu.roll(u, 32, 1))


def kernel(
    nsp,
    ntp,
    owned,
    latent,
    context,
    part,
    gain,
    wq,
    wk,
    wv,
    decay,
    head_gain,
    wo_own,
    cos,
    sin,
    out,
    lat,
    xn,
    cn,
    wq_v,
    wk_v,
    wv_v,
    wo,
    mrecv,
    mred,
    mod,
    modrow,
    q,
    k,
    v,
    ck,
    cv,
    st_send,
    st_recv,
    scan,
    en_send,
    en_recv,
    local,
    ret,
    got,
    acc,
    load_sem,
    lat_send_sem,
    lat_recv_sem,
    ms_sem,
    mr_sem,
    bs_sem,
    br_sem,
    ss_sem,
    sr_sem,
    es_sem,
    er_sem,
    gs_sem,
    gr_sem,
    wo_send_sem,
    wo_recv_sem,
):
    s = lax.axis_index("sp")
    t = lax.axis_index("tp")
    rows, dim = latent.shape
    tok = rows * ntp
    width = wq.shape[1]
    pairs = width // LANES
    crow = context.shape[0]
    nch = part.shape[0]
    owners = width // owned
    block = wo_own.shape[0]
    nz = nsp // 4
    z, y, c = s // 4, (s // 2) % 2, s % 2

    def remote(src, dst, send, recv, where):
        return pltpu.make_async_remote_copy(
            src_ref=src,
            dst_ref=dst,
            send_sem=send,
            recv_sem=recv,
            device_id=where,
            device_id_type=MESH,
        )

    loads = [
        pltpu.make_async_copy(latent, lat.at[t], load_sem.at[0]),
        pltpu.make_async_copy(wk, wk_v, load_sem.at[1]),
        pltpu.make_async_copy(wv, wv_v, load_sem.at[2]),
        pltpu.make_async_copy(wq, wq_v, load_sem.at[3]),
        pltpu.make_async_copy(wo_own, wo.at[s], load_sem.at[4]),
    ]

    def part_copy(j):
        return remote(part.at[j], mrecv.at[s], ms_sem.at[j], mr_sem.at[s], (j, t))

    for j in range(nch):
        @pl.when(s != j)
        def _():
            part_copy(j).start()

        @pl.when(s == j)
        def _():
            mrecv[j] = part[j]

    lead = rows // 4
    pieces = (pl.ds(0, lead), pl.ds(lead, rows - lead))

    def lat_copy(d, piece):
        peer = (t + d) % ntp
        return remote(
            latent.at[pieces[piece]],
            lat.at[t, pieces[piece]],
            lat_send_sem.at[d, piece],
            lat_recv_sem.at[t, piece],
            (s, peer),
        )

    for d in range(1, ntp):
        lat_copy(d, 0).start()
    for copy in loads:
        copy.start()

    def wo_copy(b, kind, src=None):
        if kind == 0:
            where = s + 4
        elif kind == 1:
            where = s - 4
        elif kind == 2:
            where = z * 4 + (1 - y) * 2 + c
        else:
            where = z * 4 + y * 2 + (1 - c)
        ref = wo.at[b] if src is None else src
        return remote(ref, wo.at[b], wo_send_sem.at[b, kind], wo_recv_sem.at[b], (where, t))

    def wo_arrived(b):
        remote(wo.at[b], wo.at[b], wo_send_sem.at[b, 0], wo_recv_sem.at[b], (s, t)).wait_recv()

    def wo_own_sends(act):
        @pl.when(z < nz - 1)
        def _():
            act(wo_copy(s, 0, wo_own))

        @pl.when(z > 0)
        def _():
            act(wo_copy(s, 1, wo_own))

        act(wo_copy(s, 2, wo_own))
        act(wo_copy(s, 3, wo_own))

    def wo_y_arrived(distance):
        def one(zz):
            b = zz * 4 + (1 - y) * 2 + c
            wo_arrived(b)
            wo_copy(b, 3).start()

        if distance == 0:
            one(z)
            return

        @pl.when(z - distance >= 0)
        def _():
            one(z - distance)

        @pl.when(z + distance < nz)
        def _():
            one(z + distance)

    furthest = jnp.maximum(z, nz - 1 - z)

    def wo_z_forward(distance, act, wait, late):
        def one(b, kind, further):
            if wait:
                wo_arrived(b)

            @pl.when(further)
            def _():
                act(wo_copy(b, kind))

            if late:
                act(wo_copy(b, 2))
            else:

                @pl.when(furthest != distance)
                def _():
                    act(wo_copy(b, 2))

            act(wo_copy(b, 3))

        @pl.when(z - distance >= 0)
        def _():
            one(s - 4 * distance, 0, z < nz - 1)

        @pl.when(z + distance < nz)
        def _():
            one(s + 4 * distance, 1, z > 0)

    def wo_step(distance):
        wo_z_forward(distance, lambda copy: copy.start(), True, False)

    def wo_late():
        for b in (s - 4 * furthest, s + 4 * furthest):
            @pl.when((b >= 0) & (b < nsp) & (furthest > 0))
            def _():
                wo_copy(b, 2).start()

    def wo_y_early(distance):
        @pl.when(furthest != distance)
        def _():
            wo_y_arrived(distance)

    def wo_y_late():
        for zz in (z - furthest, z + furthest):
            @pl.when((zz >= 0) & (zz < nz) & (furthest > 0))
            def _():
                b = zz * 4 + (1 - y) * 2 + c
                wo_arrived(b)
                wo_copy(b, 3).start()

    def to_all(act):
        def one(i):
            where = (s + i // ntp) % nsp, (t + i % ntp) % ntp

            @pl.when(i > 0)
            def _():
                act(remote(mred, mod.at[t * nch + s], bs_sem.at[i], br_sem.at[t * nch + s], where))

        loop(nsp * ntp, one)

    @pl.when(s < nch)
    def _():
        def arrived(j):
            @pl.when(j != s)
            def _():
                remote(part.at[0], mrecv.at[j], ms_sem.at[0], mr_sem.at[j], (j, t)).wait_recv()

        loop(nsp, arrived)
        total = mrecv[0]
        for j in range(1, nsp):
            total = total + mrecv[j]
        mred[...] = total
        mod[t * nch + s] = total
        to_all(lambda copy: copy.start())

    for d in range(1, ntp):
        lat_copy(d, 1).start()
    wo_own_sends(lambda copy: copy.start())

    for j in range(nch * ntp):
        @pl.when(t * nch + s != j)
        def _():
            remote(mred, mod.at[j], bs_sem.at[0], br_sem.at[j], (s, t)).wait_recv()

        @pl.when((t * nch + s == j) & (s >= nch))
        def _():
            remote(mred, mod.at[j], bs_sem.at[0], br_sem.at[j], (s, t)).wait_recv()

        modrow[:, j * LANES : (j + 1) * LANES] = mod[j]

    def normalise(src, dst, count, row):
        step = min(count, 64)

        def one(i):
            at = pl.ds(pl.multiple_of(i * step, step), step)
            x = src(at).astype(F32)
            inverse = lax.rsqrt(jnp.mean(x * x, axis=-1, keepdims=True) + EPSILON)
            dst[at, :] = (
                x * inverse * gain[...] * (1.0 + modrow[row + 1 : row + 2, :])
                + modrow[row : row + 1, :]
            ).astype(BF16)

        loop(count // step, one)

    lane_r = lax.broadcasted_iota(jnp.int32, (rows, LANES), 1)
    lane_c = lax.broadcasted_iota(jnp.int32, (crow, LANES), 1)
    tile = min(width, 256)

    normalise(lambda at: context[at, :], cn, crow, 3)
    loads[0].wait()
    loads[1].wait()
    loads[2].wait()

    def context_tile(j):
        at = pl.ds(pl.multiple_of(j * tile, tile), tile)
        kk = dot(cn[...], wk_v[:, at])
        cv[:, at] = dot(cn[...], wv_v[:, at]).astype(BF16)
        for h in range(tile // LANES):
            u = kk[:, h * LANES : (h + 1) * LANES]
            r = u * cos[pl.ds(tok, crow), :] + swap_halves(u, lane_c) * sin[pl.ds(tok, crow), :]
            ck[:, pl.ds(pl.multiple_of(j * tile + h * LANES, LANES), LANES)] = r.astype(BF16)

    loop(width // tile, context_tile)
    loads[3].wait()

    def project(d):
        src = (t + d) % ntp
        here = pl.ds(pl.multiple_of(src * rows, rows), rows)

        @pl.when(d > 0)
        def _():
            for piece in range(2):
                remote(
                    latent.at[pieces[piece]],
                    lat.at[src, pieces[piece]],
                    lat_send_sem.at[0, piece],
                    lat_recv_sem.at[src, piece],
                    (s, t),
                ).wait_recv()

        normalise(lambda at: lat[src, at, :], xn, rows, 0)

        def tile_step(j):
            at = pl.ds(pl.multiple_of(j * tile, tile), tile)
            v[here, at] = dot(xn[...], wv_v[:, at]).astype(BF16)
            cc, sn = cos[here, :], sin[here, :]
            for w_v, dst, scale in ((wk_v, k, None), (wq_v, q, HEAD ** (-0.5))):
                full = dot(xn[...], w_v[:, at])
                for h in range(tile // LANES):
                    u = full[:, h * LANES : (h + 1) * LANES]
                    r = u * cc + swap_halves(u, lane_r) * sn
                    if scale is not None:
                        r = r * scale
                    dst[here, pl.ds(pl.multiple_of(j * tile + h * LANES, LANES), LANES)] = r.astype(
                        BF16
                    )

        loop(width // tile, tile_step)

    project(0)
    near, mid = nz // 2, 3 * nz // 4
    for distance in range(1, max(near, 1)):
        wo_step(distance)
    wo_y_arrived(0)
    for distance in range(max(near, 1), max(mid, 1)):
        wo_step(distance)
    if ntp > 1:
        loop(ntp - 1, lambda d: project(d + 1))

    row_s = lax.broadcasted_iota(jnp.int32, (LANES, LANES), 0)
    lane_s = lax.broadcasted_iota(jnp.int32, (LANES, LANES), 1)
    lane_1 = lax.broadcasted_iota(jnp.int32, (1, LANES), 1)
    time_t = lax.broadcasted_iota(jnp.int32, (tok, LANES), 0).astype(F32)
    time_c = lax.broadcasted_iota(jnp.int32, (crow, LANES), 0).astype(F32)

    def rate(direction, p):
        return jnp.where(lane_1 < HEAD, decay[direction, 2 * p], decay[direction, 2 * p + 1])

    def pack(forward, backward):
        return jnp.where(
            lane_s < HEAD,
            jnp.where(row_s < HEAD, forward, pltpu.roll(forward, HEAD, 1)),
            jnp.where(row_s < HEAD, pltpu.roll(backward, HEAD, 1), backward),
        ).astype(BF16)

    def states(p):
        at = pl.ds(pl.multiple_of(p * LANES, LANES), LANES)
        ahead, behind = rate(0, p), rate(1, p)
        for which, keys, values, time in ((0, k, v, time_t), (1, ck, cv, time_c)):
            length = time.shape[0]
            kk = keys[:, at].astype(F32)
            vv = values[:, at]
            weighted = (kk * jnp.exp(ahead * (length - 1.0 - time))).astype(BF16)
            forward = dot(weighted, vv, ((0,), (0,)))
            weighted = (kk * jnp.exp(behind * time)).astype(BF16)
            backward = dot(weighted, vv, ((0,), (0,)))
            packed = pack(forward, backward)
            for i in range(LANES // owned):
                st_send[p * (LANES // owned) + i, which] = packed[i * owned : (i + 1) * owned, :]

    loop(pairs, states)

    def state_copy(j):
        return remote(st_send.at[j], st_recv.at[s], ss_sem.at[j], sr_sem.at[s], (j, t))

    def send_states(d):
        j = (s + d) % nsp

        @pl.when((j < owners) & (d > 0))
        def _():
            state_copy(j).start()

    loop(nsp, send_states)

    @pl.when(s < owners)
    def _():
        st_recv[s] = st_send[s]

    gap = (row_s - lane_s).astype(F32)
    count = tok // LANES

    def inside(p):
        at = pl.ds(pl.multiple_of(p * LANES, LANES), LANES)
        kk, vv = k[:, at], v[:, at]
        masks = []
        for a in range(2):
            ahead, behind = decay[0, 2 * p + a], decay[1, 2 * p + a]
            by_block = {0: jnp.where(gap == 0.0, 2.0, jnp.exp(jnp.where(gap > 0.0, ahead, -behind) * gap))}
            ahead_step = jnp.exp(jnp.full((1, LANES), ahead * LANES, F32))
            behind_step = jnp.exp(jnp.full((1, LANES), behind * LANES, F32))
            for n in range(1, count):
                if n == 1:
                    by_block[1] = jnp.exp(ahead * (gap + LANES))
                    by_block[-1] = jnp.exp(behind * (LANES - gap))
                else:
                    by_block[n] = by_block[n - 1] * ahead_step
                    by_block[-n] = by_block[1 - n] * behind_step
            masks.append(by_block)
        for i in range(count):
            here = slice(i * LANES, (i + 1) * LANES)
            qq = q[here, at].astype(F32)
            halves = []
            for a in range(2):
                mine = (lane_s < HEAD) if a == 0 else (lane_s >= HEAD)
                scores = dot(jnp.where(mine, qq, 0.0).astype(BF16), kk, ((1,), (1,)))
                mask = jnp.concatenate([masks[a][i - j] for j in range(count)], axis=1)
                halves.append(dot((scores * mask).astype(BF16), vv))
            local[here, at] = jnp.where(lane_s < HEAD, halves[0], halves[1])

    first = (pairs + 1) // 2
    loop(first, inside)
    for distance in range(1, max(near, 1)):
        wo_y_early(distance)

    lane_o = lax.broadcasted_iota(jnp.int32, (owned, LANES), 1)

    def enter_copy(j):
        return remote(en_send.at[j], en_recv.at[s], es_sem.at[j], er_sem.at[s], (j, t))

    @pl.when(s < owners)
    def _():
        def arrived(j):
            @pl.when(j != s)
            def _():
                remote(
                    st_send.at[0], st_recv.at[j], ss_sem.at[0], sr_sem.at[j], (j, t)
                ).wait_recv()

        loop(nsp, arrived)
        head = s * owned // HEAD
        rates = jnp.where(lane_o < HEAD, decay[0, head], decay[1, head])
        latent_step = jnp.exp(rates * float(tok))
        context_step = jnp.exp(rates * float(crow))

        def gather_forward(j, carry):
            return context_step * carry + st_recv[j, 1].astype(F32)

        def gather_backward(i, carry):
            return context_step * carry + st_recv[nsp - 1 - i, 1].astype(F32)

        zero = jnp.zeros((owned, LANES), F32)
        start = jnp.where(
            lane_o < HEAD,
            lax.fori_loop(0, nsp, gather_forward, zero),
            lax.fori_loop(0, nsp, gather_backward, zero),
        )

        def forward_step(i, carry):
            scan[i] = carry
            return latent_step * carry + st_recv[i, 0].astype(F32)

        lax.fori_loop(0, nsp, forward_step, start)

        def backward_step(n, carry):
            i = nsp - 1 - n
            en_send[i] = jnp.where(lane_o < HEAD, scan[i], carry).astype(BF16)
            return latent_step * carry + st_recv[i, 0].astype(F32)

        lax.fori_loop(0, nsp, backward_step, start)

        def send(j):
            @pl.when(j != s)
            def _():
                enter_copy(j).start()

        loop(nsp, send)
        en_recv[s] = en_send[s]

    for distance in range(max(mid, 1), nz):
        wo_step(distance)
    wo_late()
    loop(pairs - first, lambda p: inside(p + first))
    for distance in range(max(near, 1), nz):
        wo_y_early(distance)

    def entered(j):
        @pl.when(j != s)
        def _():
            remote(en_send.at[0], en_recv.at[j], es_sem.at[0], er_sem.at[j], (j, t)).wait_recv()

    loop(owners, entered)

    averaging = jnp.where((row_s < HEAD) == (lane_s < HEAD), 1.0 / HEAD, 0.0).astype(BF16)

    def head_mean(x):
        high = x.astype(BF16)
        low = (x - high.astype(F32)).astype(BF16)
        return dot(high, averaging) + dot(low, averaging)

    def ret_copy(d, p):
        peer = (t + d) % ntp
        at = pl.ds(pl.multiple_of(p * LANES, LANES), LANES)
        return remote(
            ret.at[pl.ds(pl.multiple_of(peer * rows, rows), rows), at],
            got.at[t, :, at],
            gs_sem.at[d, p],
            gr_sem.at[t, p],
            (s, peer),
        )

    def finish(p):
        at = pl.ds(pl.multiple_of(p * LANES, LANES), LANES)
        per = LANES // owned
        packed = jnp.concatenate([en_recv[p * per + i].astype(F32) for i in range(per)], axis=0)
        turned = pltpu.roll(packed, HEAD, 1)
        top = (row_s < HEAD) & (lane_s < HEAD)
        bottom = (row_s >= HEAD) & (lane_s >= HEAD)
        forward = jnp.where(top, packed, jnp.where(bottom, turned, 0.0)).astype(BF16)
        backward = jnp.where(top, turned, jnp.where(bottom, packed, 0.0)).astype(BF16)
        qq = q[:, at]
        o = (
            local[:, at]
            + dot(qq, forward) * jnp.exp(rate(0, p) * (time_t + 1.0))
            + dot(qq, backward) * jnp.exp(rate(1, p) * (float(tok) - time_t))
        )
        o = o - head_mean(o)
        spread = head_mean(o * o)
        ret[:, at] = (o * lax.rsqrt(spread + EPSILON) * head_gain[:, at]).astype(BF16)
        for d in range(1, ntp):
            ret_copy(d, p).start()
        got[t, :, at] = ret[pl.ds(pl.multiple_of(t * rows, rows), rows), at]

    loop(pairs, finish)

    wo_y_late()
    for zz in range(nz):
        for yy in range(2):
            wo_arrived(zz * 4 + yy * 2 + (1 - c))
    loads[4].wait()

    per_head_block = width // block
    cols = min(dim, 512)

    def product(src, at):
        weight = wo[pl.ds(src * per_head_block, per_head_block), :, at]
        return dot(got[src], weight.reshape(width, cols))

    def own_product(n):
        at = pl.ds(pl.multiple_of(n * cols, cols), cols)
        acc[:, at] = product(t, at)

    loop(dim // cols, own_product)
    for d in range(1, ntp):
        src = (t + d) % ntp

        def got_wait(p):
            at = pl.ds(pl.multiple_of(p * LANES, LANES), LANES)
            remote(
                ret.at[pl.ds(0, rows), at],
                got.at[src, :, at],
                gs_sem.at[0, p],
                gr_sem.at[src, p],
                (s, t),
            ).wait_recv()

        loop(pairs, got_wait)
        last = d == ntp - 1

        def peer_product(n):
            at = pl.ds(pl.multiple_of(n * cols, cols), cols)
            total = acc[:, at] + product(src, at)
            if last:
                out[:, at] = (lat[t, :, at].astype(F32) + modrow[2:3, at] * total).astype(BF16)
            else:
                acc[:, at] = total

        loop(dim // cols, peer_product)

    for j in range(nch):
        @pl.when(s != j)
        def _():
            part_copy(j).wait_send()
    for d in range(1, ntp):
        lat_copy(d, 0).wait_send()
        lat_copy(d, 1).wait_send()

    @pl.when(s < nch)
    def _():
        to_all(lambda copy: copy.wait_send())

    def states_left(d):
        j = (s + d) % nsp

        @pl.when((j < owners) & (d > 0))
        def _():
            state_copy(j).wait_send()

    loop(nsp, states_left)

    @pl.when(s < owners)
    def _():
        def left(j):
            @pl.when(j != s)
            def _():
                enter_copy(j).wait_send()

        loop(nsp, left)

    for d in range(1, ntp):
        loop(pairs, lambda p: ret_copy(d, p).wait_send())
    wo_own_sends(lambda copy: copy.wait_send())
    for distance in range(1, nz):
        wo_z_forward(distance, lambda copy: copy.wait_send(), False, True)
    for zz in range(nz):
        wo_copy(zz * 4 + (1 - y) * 2 + c, 3).wait_send()


def per_device(
    latent,
    context,
    condition,
    context_condition,
    modulation_weight,
    norm_gain,
    query_weight,
    key_weight,
    value_weight,
    log_decay,
    head_gain,
    output_weight,
):
    nsp, ntp = lax.axis_size("sp"), lax.axis_size("tp")
    s = lax.axis_index("sp")
    rows, dim = latent.shape
    tok = rows * ntp
    crow = context.shape[0]
    width = query_weight.shape[1]
    pairs = width // LANES
    owned = max(width // nsp, 16)
    owners = width // owned
    activated = jax.nn.silu(jnp.stack([condition, context_condition])).astype(BF16)
    entries, kinds, cols = modulation_weight.shape
    own_inputs = lax.dynamic_slice_in_dim(activated, s * entries, entries, 1)
    partial = jnp.einsum(
        "ce,erd->crd", own_inputs, modulation_weight, preferred_element_type=F32
    ).reshape(2 * kinds, cols)
    nch = cols // LANES
    part = jnp.pad(partial, ((0, 8 - 2 * kinds), (0, 0))).reshape(8, nch, LANES).transpose(1, 0, 2)
    place = jnp.arange(tok + crow)
    place = jnp.where(place < tok, CTX + s * tok + place, s * crow + place - tok)
    cos, sin = rotation_tables(place.astype(F32))
    vmem = pl.BlockSpec(memory_space=pltpu.VMEM)
    anywhere = pl.BlockSpec(memory_space=pl.ANY)
    smem = pl.BlockSpec(memory_space=pltpu.SMEM)
    dma = pltpu.SemaphoreType.DMA
    scratch = [
        pltpu.VMEM((ntp, rows, dim), BF16),
        pltpu.VMEM((rows, dim), BF16),
        pltpu.VMEM((crow, dim), BF16),
        pltpu.VMEM((dim, width), BF16),
        pltpu.VMEM((dim, width), BF16),
        pltpu.VMEM((dim, width), BF16),
        pltpu.VMEM((nsp,) + output_weight.shape, BF16),
        pltpu.VMEM((nsp, 8, LANES), F32),
        pltpu.VMEM((8, LANES), F32),
        pltpu.VMEM((ntp * nch, 8, LANES), F32),
        pltpu.VMEM((8, dim), F32),
        pltpu.VMEM((tok, width), BF16),
        pltpu.VMEM((tok, width), BF16),
        pltpu.VMEM((tok, width), BF16),
        pltpu.VMEM((crow, width), BF16),
        pltpu.VMEM((crow, width), BF16),
        pltpu.VMEM((owners, 2, owned, LANES), BF16),
        pltpu.VMEM((nsp, 2, owned, LANES), BF16),
        pltpu.VMEM((nsp, owned, LANES), F32),
        pltpu.VMEM((nsp, owned, LANES), BF16),
        pltpu.VMEM((owners, owned, LANES), BF16),
        pltpu.VMEM((tok, width), F32),
        pltpu.VMEM((tok, width), BF16),
        pltpu.VMEM((ntp, rows, width), BF16),
        pltpu.VMEM((rows, dim), F32),
        dma((5,)),
        dma((ntp, 2)),
        dma((ntp, 2)),
        dma((nch,)),
        dma((nsp,)),
        dma((nsp * ntp,)),
        dma((ntp * nch,)),
        dma((owners,)),
        dma((nsp,)),
        dma((nsp,)),
        dma((owners,)),
        dma((ntp, pairs)),
        dma((ntp, pairs)),
        dma((nsp, 4)),
        dma((nsp,)),
    ]
    return pl.pallas_call(
        functools.partial(kernel, nsp, ntp, owned),
        out_shape=jax.ShapeDtypeStruct((rows, dim), BF16),
        in_specs=[anywhere, vmem, vmem, vmem, anywhere, anywhere, anywhere, smem]
        + [vmem, anywhere, vmem, vmem],
        out_specs=vmem,
        scratch_shapes=scratch,
        compiler_params=pltpu.CompilerParams(
            has_side_effects=True, vmem_limit_bytes=66_000_000
        ),
    )(
        latent,
        context,
        part,
        norm_gain[None],
        query_weight,
        key_weight,
        value_weight,
        log_decay,
        head_gain[None],
        output_weight,
        cos,
        sin,
    )


def solution(mesh):
    in_specs = (
        P(("sp", "tp"), None),
        P("sp", None),
        P(),
        P(),
        P("sp", None, "tp"),
        P(),
        P(None, "tp"),
        P(None, "tp"),
        P(None, "tp"),
        P(None, "tp"),
        P("tp"),
        P("sp", None),
    )
    out_specs = P(("sp", "tp"), None)
    return jax.shard_map(
        per_device, mesh=mesh, in_specs=in_specs, out_specs=out_specs, check_vma=False
    )
```

```python
import functools

import jax
import jax.numpy as jnp
from jax import lax
from jax.experimental import pallas as pl
from jax.experimental.pallas import tpu as pltpu
from jax.sharding import PartitionSpec as P

HEAD = 64
CTX = 1024
LANES = 128
EPSILON = 1e-06
ROTARY_BASE = 10000.0
MESH = pl.DeviceIdType.MESH
F32 = jnp.float32
BF16 = jnp.bfloat16


def rotation_tables(positions):
    half_size = HEAD // 2
    frequency = 1.0 / ROTARY_BASE ** jnp.linspace(0.0, 1.0, half_size, dtype=F32)
    lane = jnp.arange(LANES)
    angles = positions[:, None] * jnp.tile(frequency, LANES // half_size)[None, :]
    sign = jnp.where(lane % HEAD < half_size, -1.0, 1.0).astype(F32)
    return jnp.cos(angles), jnp.sin(angles) * sign[None, :]


def dot(a, b, dims=((1,), (0,))):
    return lax.dot_general(a, b, (dims, ((), ())), preferred_element_type=F32)


def loop(count, body):
    def step(i, carry):
        body(i)
        return carry

    lax.fori_loop(0, count, step, 0)


def swap_halves(u, lane):
    return jnp.where(lane % HEAD < HEAD // 2, pltpu.roll(u, LANES - 32, 1), pltpu.roll(u, 32, 1))


def kernel(
    nsp,
    ntp,
    owned,
    latent,
    context,
    part,
    gain,
    wq,
    wk,
    wv,
    decay,
    head_gain,
    wo_own,
    cos,
    sin,
    out,
    lat,
    xn,
    cn,
    wq_v,
    wk_v,
    wv_v,
    wo,
    mrecv,
    mred,
    mod,
    modrow,
    q,
    k,
    v,
    ck,
    cv,
    st_send,
    st_recv,
    scan,
    en_send,
    en_recv,
    local,
    ret,
    got,
    acc,
    load_sem,
    lat_send_sem,
    lat_recv_sem,
    ms_sem,
    mr_sem,
    bs_sem,
    br_sem,
    ss_sem,
    sr_sem,
    es_sem,
    er_sem,
    gs_sem,
    gr_sem,
    wo_send_sem,
    wo_recv_sem,
):
    s = lax.axis_index("sp")
    t = lax.axis_index("tp")
    rows, dim = latent.shape
    tok = rows * ntp
    width = wq.shape[1]
    pairs = width // LANES
    crow = context.shape[0]
    nch = part.shape[0]
    owners = width // owned
    block = wo_own.shape[0]
    nz = nsp // 4
    z, y, c = s // 4, (s // 2) % 2, s % 2

    def remote(src, dst, send, recv, where):
        return pltpu.make_async_remote_copy(
            src_ref=src,
            dst_ref=dst,
            send_sem=send,
            recv_sem=recv,
            device_id=where,
            device_id_type=MESH,
        )

    loads = [
        pltpu.make_async_copy(latent, lat.at[t], load_sem.at[0]),
        pltpu.make_async_copy(wk, wk_v, load_sem.at[1]),
        pltpu.make_async_copy(wv, wv_v, load_sem.at[2]),
        pltpu.make_async_copy(wq, wq_v, load_sem.at[3]),
        pltpu.make_async_copy(wo_own, wo.at[s], load_sem.at[4]),
    ]

    def part_copy(j):
        return remote(part.at[j], mrecv.at[s], ms_sem.at[j], mr_sem.at[s], (j, t))

    for j in range(nch):
        @pl.when(s != j)
        def _():
            part_copy(j).start()

        @pl.when(s == j)
        def _():
            mrecv[j] = part[j]

    lead = rows // 4
    pieces = (pl.ds(0, lead), pl.ds(lead, rows - lead))

    def lat_copy(d, piece):
        peer = (t + d) % ntp
        return remote(
            latent.at[pieces[piece]],
            lat.at[t, pieces[piece]],
            lat_send_sem.at[d, piece],
            lat_recv_sem.at[t, piece],
            (s, peer),
        )

    for d in range(1, ntp):
        lat_copy(d, 0).start()
    for copy in loads:
        copy.start()

    def wo_copy(b, kind, src=None):
        if kind == 0:
            where = s + 4
        elif kind == 1:
            where = s - 4
        elif kind == 2:
            where = z * 4 + (1 - y) * 2 + c
        else:
            where = z * 4 + y * 2 + (1 - c)
        ref = wo.at[b] if src is None else src
        return remote(ref, wo.at[b], wo_send_sem.at[b, kind], wo_recv_sem.at[b], (where, t))

    def wo_arrived(b):
        remote(wo.at[b], wo.at[b], wo_send_sem.at[b, 0], wo_recv_sem.at[b], (s, t)).wait_recv()

    def wo_own_sends(act):
        @pl.when(z < nz - 1)
        def _():
            act(wo_copy(s, 0, wo_own))

        @pl.when(z > 0)
        def _():
            act(wo_copy(s, 1, wo_own))

        act(wo_copy(s, 2, wo_own))
        act(wo_copy(s, 3, wo_own))

    def wo_y_arrived(distance):
        def one(zz):
            b = zz * 4 + (1 - y) * 2 + c
            wo_arrived(b)
            wo_copy(b, 3).start()

        if distance == 0:
            one(z)
            return

        @pl.when(z - distance >= 0)
        def _():
            one(z - distance)

        @pl.when(z + distance < nz)
        def _():
            one(z + distance)

    furthest = jnp.maximum(z, nz - 1 - z)

    def wo_z_forward(distance, act, wait, late):
        def one(b, kind, further):
            if wait:
                wo_arrived(b)

            @pl.when(further)
            def _():
                act(wo_copy(b, kind))

            if late:
                act(wo_copy(b, 2))
            else:

                @pl.when(furthest != distance)
                def _():
                    act(wo_copy(b, 2))

            act(wo_copy(b, 3))

        @pl.when(z - distance >= 0)
        def _():
            one(s - 4 * distance, 0, z < nz - 1)

        @pl.when(z + distance < nz)
        def _():
            one(s + 4 * distance, 1, z > 0)

    def wo_step(distance):
        wo_z_forward(distance, lambda copy: copy.start(), True, False)

    def wo_late():
        for b in (s - 4 * furthest, s + 4 * furthest):
            @pl.when((b >= 0) & (b < nsp) & (furthest > 0))
            def _():
                wo_copy(b, 2).start()

    def wo_y_early(distance):
        @pl.when(furthest != distance)
        def _():
            wo_y_arrived(distance)

    def wo_y_late():
        for zz in (z - furthest, z + furthest):
            @pl.when((zz >= 0) & (zz < nz) & (furthest > 0))
            def _():
                b = zz * 4 + (1 - y) * 2 + c
                wo_arrived(b)
                wo_copy(b, 3).start()

    def to_all(act):
        def one(i):
            where = (s + i // ntp) % nsp, (t + i % ntp) % ntp

            @pl.when(i > 0)
            def _():
                act(remote(mred, mod.at[t * nch + s], bs_sem.at[i], br_sem.at[t * nch + s], where))

        loop(nsp * ntp, one)

    @pl.when(s < nch)
    def _():
        def arrived(j):
            @pl.when(j != s)
            def _():
                remote(part.at[0], mrecv.at[j], ms_sem.at[0], mr_sem.at[j], (j, t)).wait_recv()

        loop(nsp, arrived)
        total = mrecv[0]
        for j in range(1, nsp):
            total = total + mrecv[j]
        mred[...] = total
        mod[t * nch + s] = total
        to_all(lambda copy: copy.start())

    for d in range(1, ntp):
        lat_copy(d, 1).start()
    wo_own_sends(lambda copy: copy.start())

    for j in range(nch * ntp):
        @pl.when(t * nch + s != j)
        def _():
            remote(mred, mod.at[j], bs_sem.at[0], br_sem.at[j], (s, t)).wait_recv()

        @pl.when((t * nch + s == j) & (s >= nch))
        def _():
            remote(mred, mod.at[j], bs_sem.at[0], br_sem.at[j], (s, t)).wait_recv()

        modrow[:, j * LANES : (j + 1) * LANES] = mod[j]

    def normalise(src, dst, count, row):
        step = min(count, 64)

        def one(i):
            at = pl.ds(pl.multiple_of(i * step, step), step)
            x = src(at).astype(F32)
            inverse = lax.rsqrt(jnp.mean(x * x, axis=-1, keepdims=True) + EPSILON)
            dst[at, :] = (
                x * inverse * gain[...] * (1.0 + modrow[row + 1 : row + 2, :])
                + modrow[row : row + 1, :]
            ).astype(BF16)

        loop(count // step, one)

    lane_r = lax.broadcasted_iota(jnp.int32, (rows, LANES), 1)
    lane_c = lax.broadcasted_iota(jnp.int32, (crow, LANES), 1)
    tile = min(width, 256)

    normalise(lambda at: context[at, :], cn, crow, 3)
    loads[0].wait()
    loads[1].wait()
    loads[2].wait()

    def context_tile(j):
        at = pl.ds(pl.multiple_of(j * tile, tile), tile)
        kk = dot(cn[...], wk_v[:, at])
        cv[:, at] = dot(cn[...], wv_v[:, at]).astype(BF16)
        for h in range(tile // LANES):
            u = kk[:, h * LANES : (h + 1) * LANES]
            r = u * cos[pl.ds(tok, crow), :] + swap_halves(u, lane_c) * sin[pl.ds(tok, crow), :]
            ck[:, pl.ds(pl.multiple_of(j * tile + h * LANES, LANES), LANES)] = r.astype(BF16)

    loop(width // tile, context_tile)
    loads[3].wait()

    def project(d):
        src = (t + d) % ntp
        here = pl.ds(pl.multiple_of(src * rows, rows), rows)

        @pl.when(d > 0)
        def _():
            for piece in range(2):
                remote(
                    latent.at[pieces[piece]],
                    lat.at[src, pieces[piece]],
                    lat_send_sem.at[0, piece],
                    lat_recv_sem.at[src, piece],
                    (s, t),
                ).wait_recv()

        normalise(lambda at: lat[src, at, :], xn, rows, 0)

        def tile_step(j):
            at = pl.ds(pl.multiple_of(j * tile, tile), tile)
            v[here, at] = dot(xn[...], wv_v[:, at]).astype(BF16)
            cc, sn = cos[here, :], sin[here, :]
            for w_v, dst, scale in ((wk_v, k, None), (wq_v, q, HEAD ** (-0.5))):
                full = dot(xn[...], w_v[:, at])
                for h in range(tile // LANES):
                    u = full[:, h * LANES : (h + 1) * LANES]
                    r = u * cc + swap_halves(u, lane_r) * sn
                    if scale is not None:
                        r = r * scale
                    dst[here, pl.ds(pl.multiple_of(j * tile + h * LANES, LANES), LANES)] = r.astype(
                        BF16
                    )

        loop(width // tile, tile_step)

    project(0)
    near, mid = nz // 2, 3 * nz // 4
    for distance in range(1, max(near, 1)):
        wo_step(distance)
    wo_y_arrived(0)
    for distance in range(max(near, 1), max(mid, 1)):
        wo_step(distance)
    if ntp > 1:
        loop(ntp - 1, lambda d: project(d + 1))

    row_s = lax.broadcasted_iota(jnp.int32, (LANES, LANES), 0)
    lane_s = lax.broadcasted_iota(jnp.int32, (LANES, LANES), 1)
    lane_1 = lax.broadcasted_iota(jnp.int32, (1, LANES), 1)
    time_t = lax.broadcasted_iota(jnp.int32, (tok, LANES), 0).astype(F32)
    time_c = lax.broadcasted_iota(jnp.int32, (crow, LANES), 0).astype(F32)

    def rate(direction, p):
        return jnp.where(lane_1 < HEAD, decay[direction, 2 * p], decay[direction, 2 * p + 1])

    def pack(forward, backward):
        return jnp.where(
            lane_s < HEAD,
            jnp.where(row_s < HEAD, forward, pltpu.roll(forward, HEAD, 1)),
            jnp.where(row_s < HEAD, pltpu.roll(backward, HEAD, 1), backward),
        ).astype(BF16)

    def states(p):
        at = pl.ds(pl.multiple_of(p * LANES, LANES), LANES)
        ahead, behind = rate(0, p), rate(1, p)
        for which, keys, values, time in ((0, k, v, time_t), (1, ck, cv, time_c)):
            length = time.shape[0]
            kk = keys[:, at].astype(F32)
            vv = values[:, at]
            weighted = (kk * jnp.exp(ahead * (length - 1.0 - time))).astype(BF16)
            forward = dot(weighted, vv, ((0,), (0,)))
            weighted = (kk * jnp.exp(behind * time)).astype(BF16)
            backward = dot(weighted, vv, ((0,), (0,)))
            packed = pack(forward, backward)
            for i in range(LANES // owned):
                st_send[p * (LANES // owned) + i, which] = packed[i * owned : (i + 1) * owned, :]

    loop(pairs, states)

    def state_copy(j):
        return remote(st_send.at[j], st_recv.at[s], ss_sem.at[j], sr_sem.at[s], (j, t))

    def send_states(d):
        j = (s + d) % nsp

        @pl.when((j < owners) & (d > 0))
        def _():
            state_copy(j).start()

    loop(nsp, send_states)

    @pl.when(s < owners)
    def _():
        st_recv[s] = st_send[s]

    gap = (row_s - lane_s).astype(F32)
    count = tok // LANES

    def inside(p):
        at = pl.ds(pl.multiple_of(p * LANES, LANES), LANES)
        kk, vv = k[:, at], v[:, at]
        masks = []
        for a in range(2):
            ahead, behind = decay[0, 2 * p + a], decay[1, 2 * p + a]
            by_block = {0: jnp.where(gap == 0.0, 2.0, jnp.exp(jnp.where(gap > 0.0, ahead, -behind) * gap))}
            ahead_step = jnp.exp(jnp.full((1, LANES), ahead * LANES, F32))
            behind_step = jnp.exp(jnp.full((1, LANES), behind * LANES, F32))
            for n in range(1, count):
                if n == 1:
                    by_block[1] = jnp.exp(ahead * (gap + LANES))
                    by_block[-1] = jnp.exp(behind * (LANES - gap))
                else:
                    by_block[n] = by_block[n - 1] * ahead_step
                    by_block[-n] = by_block[1 - n] * behind_step
            masks.append(by_block)
        for i in range(count):
            here = slice(i * LANES, (i + 1) * LANES)
            qq = q[here, at].astype(F32)
            halves = []
            for a in range(2):
                mine = (lane_s < HEAD) if a == 0 else (lane_s >= HEAD)
                scores = dot(jnp.where(mine, qq, 0.0).astype(BF16), kk, ((1,), (1,)))
                mask = jnp.concatenate([masks[a][i - j] for j in range(count)], axis=1)
                halves.append(dot((scores * mask).astype(BF16), vv))
            local[here, at] = jnp.where(lane_s < HEAD, halves[0], halves[1])

    first = (pairs + 1) // 2
    loop(first, inside)
    for distance in range(1, max(near, 1)):
        wo_y_early(distance)

    lane_o = lax.broadcasted_iota(jnp.int32, (owned, LANES), 1)

    def enter_copy(j):
        return remote(en_send.at[j], en_recv.at[s], es_sem.at[j], er_sem.at[s], (j, t))

    @pl.when(s < owners)
    def _():
        def arrived(j):
            @pl.when(j != s)
            def _():
                remote(
                    st_send.at[0], st_recv.at[j], ss_sem.at[0], sr_sem.at[j], (j, t)
                ).wait_recv()

        loop(nsp, arrived)
        head = s * owned // HEAD
        rates = jnp.where(lane_o < HEAD, decay[0, head], decay[1, head])
        latent_step = jnp.exp(rates * float(tok))
        context_step = jnp.exp(rates * float(crow))

        def gather_forward(j, carry):
            return context_step * carry + st_recv[j, 1].astype(F32)

        def gather_backward(i, carry):
            return context_step * carry + st_recv[nsp - 1 - i, 1].astype(F32)

        zero = jnp.zeros((owned, LANES), F32)
        start = jnp.where(
            lane_o < HEAD,
            lax.fori_loop(0, nsp, gather_forward, zero),
            lax.fori_loop(0, nsp, gather_backward, zero),
        )

        def forward_step(i, carry):
            scan[i] = carry
            return latent_step * carry + st_recv[i, 0].astype(F32)

        lax.fori_loop(0, nsp, forward_step, start)

        def backward_step(n, carry):
            i = nsp - 1 - n
            en_send[i] = jnp.where(lane_o < HEAD, scan[i], carry).astype(BF16)
            return latent_step * carry + st_recv[i, 0].astype(F32)

        lax.fori_loop(0, nsp, backward_step, start)

        def send(j):
            @pl.when(j != s)
            def _():
                enter_copy(j).start()

        loop(nsp, send)
        en_recv[s] = en_send[s]

    for distance in range(max(mid, 1), nz):
        wo_step(distance)
    wo_late()
    loop(pairs - first, lambda p: inside(p + first))
    for distance in range(max(near, 1), nz):
        wo_y_early(distance)

    def entered(j):
        @pl.when(j != s)
        def _():
            remote(en_send.at[0], en_recv.at[j], es_sem.at[0], er_sem.at[j], (j, t)).wait_recv()

    loop(owners, entered)

    averaging = jnp.where((row_s < HEAD) == (lane_s < HEAD), 1.0 / HEAD, 0.0).astype(BF16)

    def head_mean(x):
        high = x.astype(BF16)
        low = (x - high.astype(F32)).astype(BF16)
        return dot(high, averaging) + dot(low, averaging)

    def ret_copy(d, p):
        peer = (t + d) % ntp
        at = pl.ds(pl.multiple_of(p * LANES, LANES), LANES)
        return remote(
            ret.at[pl.ds(pl.multiple_of(peer * rows, rows), rows), at],
            got.at[t, :, at],
            gs_sem.at[d, p],
            gr_sem.at[t, p],
            (s, peer),
        )

    def finish(p):
        at = pl.ds(pl.multiple_of(p * LANES, LANES), LANES)
        per = LANES // owned
        packed = jnp.concatenate([en_recv[p * per + i].astype(F32) for i in range(per)], axis=0)
        turned = pltpu.roll(packed, HEAD, 1)
        top = (row_s < HEAD) & (lane_s < HEAD)
        bottom = (row_s >= HEAD) & (lane_s >= HEAD)
        forward = jnp.where(top, packed, jnp.where(bottom, turned, 0.0)).astype(BF16)
        backward = jnp.where(top, turned, jnp.where(bottom, packed, 0.0)).astype(BF16)
        qq = q[:, at]
        o = (
            local[:, at]
            + dot(qq, forward) * jnp.exp(rate(0, p) * (time_t + 1.0))
            + dot(qq, backward) * jnp.exp(rate(1, p) * (float(tok) - time_t))
        )
        o = o - head_mean(o)
        spread = head_mean(o * o)
        ret[:, at] = (o * lax.rsqrt(spread + EPSILON) * head_gain[:, at]).astype(BF16)
        for d in range(1, ntp):
            ret_copy(d, p).start()
        got[t, :, at] = ret[pl.ds(pl.multiple_of(t * rows, rows), rows), at]

    loop(pairs, finish)

    wo_y_late()
    loads[4].wait()
    per_head_block = width // block

    def weight_rows(src):
        for i in range(per_head_block // 2):
            wo_arrived(src * per_head_block + 2 * i + (1 - c))

    weight_rows(t)
    cols = min(dim, 512)

    def product(src, at):
        weight = wo[pl.ds(src * per_head_block, per_head_block), :, at]
        return dot(got[src], weight.reshape(width, cols))

    def own_product(n):
        at = pl.ds(pl.multiple_of(n * cols, cols), cols)
        acc[:, at] = product(t, at)

    loop(dim // cols, own_product)
    for d in range(1, ntp):
        src = (t + d) % ntp

        def got_wait(p):
            at = pl.ds(pl.multiple_of(p * LANES, LANES), LANES)
            remote(
                ret.at[pl.ds(0, rows), at],
                got.at[src, :, at],
                gs_sem.at[0, p],
                gr_sem.at[src, p],
                (s, t),
            ).wait_recv()

        weight_rows(src)
        loop(pairs, got_wait)
        last = d == ntp - 1

        def peer_product(n):
            at = pl.ds(pl.multiple_of(n * cols, cols), cols)
            total = acc[:, at] + product(src, at)
            if last:
                out[:, at] = (lat[t, :, at].astype(F32) + modrow[2:3, at] * total).astype(BF16)
            else:
                acc[:, at] = total

        loop(dim // cols, peer_product)

    for j in range(nch):
        @pl.when(s != j)
        def _():
            part_copy(j).wait_send()
    for d in range(1, ntp):
        lat_copy(d, 0).wait_send()
        lat_copy(d, 1).wait_send()

    @pl.when(s < nch)
    def _():
        to_all(lambda copy: copy.wait_send())

    def states_left(d):
        j = (s + d) % nsp

        @pl.when((j < owners) & (d > 0))
        def _():
            state_copy(j).wait_send()

    loop(nsp, states_left)

    @pl.when(s < owners)
    def _():
        def left(j):
            @pl.when(j != s)
            def _():
                enter_copy(j).wait_send()

        loop(nsp, left)

    for d in range(1, ntp):
        loop(pairs, lambda p: ret_copy(d, p).wait_send())
    wo_own_sends(lambda copy: copy.wait_send())
    for distance in range(1, nz):
        wo_z_forward(distance, lambda copy: copy.wait_send(), False, True)
    for zz in range(nz):
        wo_copy(zz * 4 + (1 - y) * 2 + c, 3).wait_send()


def per_device(
    latent,
    context,
    condition,
    context_condition,
    modulation_weight,
    norm_gain,
    query_weight,
    key_weight,
    value_weight,
    log_decay,
    head_gain,
    output_weight,
):
    nsp, ntp = lax.axis_size("sp"), lax.axis_size("tp")
    s = lax.axis_index("sp")
    rows, dim = latent.shape
    tok = rows * ntp
    crow = context.shape[0]
    width = query_weight.shape[1]
    pairs = width // LANES
    owned = max(width // nsp, 16)
    owners = width // owned
    activated = jax.nn.silu(jnp.stack([condition, context_condition])).astype(BF16)
    entries, kinds, cols = modulation_weight.shape
    own_inputs = lax.dynamic_slice_in_dim(activated, s * entries, entries, 1)
    partial = jnp.einsum(
        "ce,erd->crd", own_inputs, modulation_weight, preferred_element_type=F32
    ).reshape(2 * kinds, cols)
    nch = cols // LANES
    part = jnp.pad(partial, ((0, 8 - 2 * kinds), (0, 0))).reshape(8, nch, LANES).transpose(1, 0, 2)
    place = jnp.arange(tok + crow)
    place = jnp.where(place < tok, CTX + s * tok + place, s * crow + place - tok)
    cos, sin = rotation_tables(place.astype(F32))
    vmem = pl.BlockSpec(memory_space=pltpu.VMEM)
    anywhere = pl.BlockSpec(memory_space=pl.ANY)
    smem = pl.BlockSpec(memory_space=pltpu.SMEM)
    dma = pltpu.SemaphoreType.DMA
    scratch = [
        pltpu.VMEM((ntp, rows, dim), BF16),
        pltpu.VMEM((rows, dim), BF16),
        pltpu.VMEM((crow, dim), BF16),
        pltpu.VMEM((dim, width), BF16),
        pltpu.VMEM((dim, width), BF16),
        pltpu.VMEM((dim, width), BF16),
        pltpu.VMEM((nsp,) + output_weight.shape, BF16),
        pltpu.VMEM((nsp, 8, LANES), F32),
        pltpu.VMEM((8, LANES), F32),
        pltpu.VMEM((ntp * nch, 8, LANES), F32),
        pltpu.VMEM((8, dim), F32),
        pltpu.VMEM((tok, width), BF16),
        pltpu.VMEM((tok, width), BF16),
        pltpu.VMEM((tok, width), BF16),
        pltpu.VMEM((crow, width), BF16),
        pltpu.VMEM((crow, width), BF16),
        pltpu.VMEM((owners, 2, owned, LANES), BF16),
        pltpu.VMEM((nsp, 2, owned, LANES), BF16),
        pltpu.VMEM((nsp, owned, LANES), F32),
        pltpu.VMEM((nsp, owned, LANES), BF16),
        pltpu.VMEM((owners, owned, LANES), BF16),
        pltpu.VMEM((tok, width), F32),
        pltpu.VMEM((tok, width), BF16),
        pltpu.VMEM((ntp, rows, width), BF16),
        pltpu.VMEM((rows, dim), F32),
        dma((5,)),
        dma((ntp, 2)),
        dma((ntp, 2)),
        dma((nch,)),
        dma((nsp,)),
        dma((nsp * ntp,)),
        dma((ntp * nch,)),
        dma((owners,)),
        dma((nsp,)),
        dma((nsp,)),
        dma((owners,)),
        dma((ntp, pairs)),
        dma((ntp, pairs)),
        dma((nsp, 4)),
        dma((nsp,)),
    ]
    return pl.pallas_call(
        functools.partial(kernel, nsp, ntp, owned),
        out_shape=jax.ShapeDtypeStruct((rows, dim), BF16),
        in_specs=[anywhere, vmem, vmem, vmem, anywhere, anywhere, anywhere, smem]
        + [vmem, anywhere, vmem, vmem],
        out_specs=vmem,
        scratch_shapes=scratch,
        compiler_params=pltpu.CompilerParams(
            has_side_effects=True, vmem_limit_bytes=66_000_000
        ),
    )(
        latent,
        context,
        part,
        norm_gain[None],
        query_weight,
        key_weight,
        value_weight,
        log_decay,
        head_gain[None],
        output_weight,
        cos,
        sin,
    )


def solution(mesh):
    in_specs = (
        P(("sp", "tp"), None),
        P("sp", None),
        P(),
        P(),
        P("sp", None, "tp"),
        P(),
        P(None, "tp"),
        P(None, "tp"),
        P(None, "tp"),
        P(None, "tp"),
        P("tp"),
        P("sp", None),
    )
    out_specs = P(("sp", "tp"), None)
    return jax.shard_map(
        per_device, mesh=mesh, in_specs=in_specs, out_specs=out_specs, check_vma=False
    )
```
